512 devices in a mesh: sp: 64 (over z, y), dp: 8 (over x, core).
Axes of the slice: x: 4, y: 4, z: 16, core: 2. Of those that a mesh axis runs over, the one named last changes fastest.
Arguments:
- gate_input: bfloat16 [8, 12288, 4096], P('dp', 'sp'), may hold values from -6 to 6
- value_input: bfloat16 [8, 12288, 4096], P('dp', 'sp'), may hold values from -6 to 6
- norm_gain: float32 [4096], replicated, may hold values from 0.1 to 1.9
- norm_bias: float32 [4096], replicated, may hold values from -3 to 3
- mix_weight: bfloat16 [64, 1024, 1024], P('sp', 'dp'), may hold values from -0.1875 to 0.1875
- mix_bias: float32 [64, 1024], P('sp'), may hold values from 0.1 to 1.9
Outputs:
- gated: bfloat16 [8, 12288, 4096], P('dp', 'sp')
The draws below stay inside these ranges and needn't reach their ends.
All inputs are finite; a program needn't handle non-finite values.
Results may differ from the reference program's by a relative error of at most 0.0053.
Values may be sent and summed in bfloat16 or wider, within the bound.
No kernel may reach another device: no remote copies, remote signals or barrier semaphores. Data moves between devices by JAX's collectives and lax.ppermute only.
A program may use at most 64 MiB of HBM per device.

```python
import jax
import jax.numpy as jnp
from jax import lax

GROUP_DIM = 64
SPAN = 1024
GROUPS = 64
WIDTH = 4096
SEQ = 12288
BATCH = 8


def shard_levels(own_key, dims, shards, least, largest):
    def one(position, blocks):
        steps = jax.random.uniform(jax.random.fold_in(jax.random.fold_in(own_key, 6), position), (blocks,), jnp.float32, least / len(shards), largest / len(shards))
        return jnp.repeat(jnp.exp(steps), dims[position] // blocks).reshape((-1,) + (1,) * (len(dims) - position - 1))

    loudness = one(*shards[0])
    for cut in shards[1:]:
        loudness = loudness * one(*cut)
    return loudness


def gaussian(own_key, shape, width, limit, cuts=(), dtype=jnp.bfloat16):
    drawn = jax.random.normal(own_key, shape, jnp.float32) * width
    if len(cuts) > 0:
        drawn = shard_levels(own_key, shape, cuts, -0.22, 0.18) * drawn
    return jnp.clip(drawn, min=-limit, max=limit).astype(dtype)


def setup_inputs(seed: int = 0) -> dict:
    key_list = jax.random.split(jax.random.key(seed), 7)
    gate_input = gaussian(key_list[0], (BATCH, SEQ, WIDTH), 1.0, 6.0, ((0, 8), (1, 64)))
    value_input = gaussian(key_list[1], (BATCH, SEQ, WIDTH), 1.0, 6.0, ((0, 8), (1, 64)))
    norm_gain = jnp.clip(1.0 + 0.18 * jax.random.normal(key_list[2], (WIDTH,), jnp.float32), 0.1, 1.9)
    norm_bias = gaussian(key_list[3], (WIDTH,), 0.5, 3.0, (), jnp.float32)
    mix_weight = gaussian(key_list[4], (GROUPS, SPAN, SPAN), SPAN ** -0.5, 0.1875, ((0, 64), (1, 8)))
    mix_bias = jnp.clip(1.0 + 0.18 * jax.random.normal(key_list[5], (GROUPS, SPAN), jnp.float32), 0.1, 1.9)
    return dict(gate_input=gate_input, value_input=value_input, norm_gain=norm_gain, norm_bias=norm_bias, mix_weight=mix_weight, mix_bias=mix_bias)


epsilon = 1e-05

def reference(gate_input, value_input, norm_gain, norm_bias, mix_weight, mix_bias):
    causal = jnp.tril(jnp.ones((SPAN, SPAN), jnp.float32))
    weight = mix_weight.astype(jnp.float32) * causal[None]

    def per_sequence(inputs):
        gate_rows, value_rows = inputs
        act_value = jax.nn.gelu(value_rows.astype(jnp.float32))
        centre = lax.optimization_barrier(jnp.mean(act_value, axis=-1, keepdims=True))
        shifted = act_value - centre
        variance = lax.optimization_barrier(jnp.mean(shifted * shifted, axis=-1, keepdims=True))
        normed = (shifted * lax.rsqrt(variance + epsilon) * norm_gain + norm_bias).astype(jnp.bfloat16)
        blocks = normed.astype(jnp.float32).reshape(SEQ // SPAN, SPAN, GROUPS, GROUP_DIM)
        summed = jnp.einsum('gqp,npgc->nqgc', weight, blocks, precision=lax.Precision.HIGHEST)
        mixed_rows = (summed + mix_bias.T[None, :, :, None]).reshape(SEQ, WIDTH).astype(jnp.bfloat16)
        mixed_rows = lax.optimization_barrier(mixed_rows)
        act_gate = jax.nn.gelu(gate_rows.astype(jnp.float32))
        return (act_gate * mixed_rows.astype(jnp.float32)).astype(jnp.bfloat16)
    return lax.map(per_sequence, (gate_input, value_input))
```

```python
import jax
import jax.numpy as jnp
from jax import lax
from jax.experimental import pallas as pl
from jax.experimental.pallas import tpu as pltpu
from jax.sharding import Mesh
from jax.sharding import PartitionSpec as P

GROUP_DIM = 64
SPAN = 1024
TILE = 128
EPSILON = 1e-05
QUAD = ("x", "zr", "y")

VMEM = pl.BlockSpec(memory_space=pltpu.VMEM)
SMEM = pl.BlockSpec(memory_space=pltpu.SMEM)


def lane_is_low(shape):
    return lax.broadcasted_iota(jnp.int32, shape, 1) < GROUP_DIM


def swap_halves(upper, lower):
    low = lane_is_low(upper.shape)
    first = jnp.where(low, upper, pltpu.roll(lower, GROUP_DIM, 1))
    second = jnp.where(low, pltpu.roll(upper, GROUP_DIM, 1), lower)
    return first, second


def norm_kernel(value_ref, gain_ref, bias_ref, out_ref, act_ref):
    rows, channels = value_ref.shape
    half = rows // 2
    step = 16
    tiles = channels // TILE

    def chunk(i, carry):
        top = pl.ds(pl.multiple_of(i * step, step), step)
        bottom = pl.ds(pl.multiple_of(half + i * step, step), step)
        total = jnp.zeros((2 * step, TILE), jnp.float32)
        for t in range(tiles):
            lanes = pl.ds(t * TILE, TILE)
            both = jnp.concatenate([value_ref[top, lanes], value_ref[bottom, lanes]], axis=0)
            act = jax.nn.gelu(both.astype(jnp.float32))
            act_ref[:, lanes] = act
            total = total + act
        centre = jnp.sum(total, axis=1, keepdims=True) * (1.0 / channels)
        square = jnp.zeros((2 * step, TILE), jnp.float32)
        for t in range(tiles):
            shifted = act_ref[:, pl.ds(t * TILE, TILE)] - centre
            square = square + shifted * shifted
        variance = jnp.sum(square, axis=1, keepdims=True) * (1.0 / channels)
        scale = lax.rsqrt(variance + EPSILON)
        for t in range(tiles):
            lanes = pl.ds(t * TILE, TILE)
            shifted = act_ref[:, lanes] - centre
            normed = shifted * scale * gain_ref[:, lanes] + bias_ref[:, lanes]
            first, second = swap_halves(normed[:step], normed[step:])
            out_ref[2 * t, top, :] = first.astype(out_ref.dtype)
            out_ref[2 * t + 1, top, :] = second.astype(out_ref.dtype)
        return carry

    lax.fori_loop(0, half // step, chunk, 0)


def fold_kernel(place_ref, weight_ref, excess_ref, bias_ref, out_ref):
    d = place_ref[0]
    for b in range(5):
        block = weight_ref[:, b * TILE : (b + 1) * TILE]
        if b >= 2:
            e = 4 - b
            block = jnp.where(b >= d + 2, excess_ref[:, e * TILE : (e + 1) * TILE], block)
        out_ref[b * TILE : (b + 1) * TILE, :] = block
    bias = bias_ref[pl.ds(d, 1), :]
    high = bias.astype(jnp.bfloat16).astype(jnp.float32)
    low = bias - high
    row = lax.broadcasted_iota(jnp.int32, (16, TILE), 0)
    pair = jnp.where(row == 0, high, jnp.where(row == 1, low, 0.0))
    out_ref[5 * TILE :, :] = pair.astype(out_ref.dtype)


def mix_kernel(place_ref, acts_ref, own_ref, other_ref, out_ref, weight, stack):
    quad, core = place_ref[0], place_ref[1]
    pieces, half, _ = acts_ref.shape[1:]

    def unpack(k, carry):
        upper = pl.ds(pl.multiple_of(k * 2 * half, 2 * half), half)
        lower = pl.ds(pl.multiple_of(k * 2 * half + half, half), half)
        for pair in range(2):
            lanes = pl.ds(pair * TILE, TILE)
            first, second = swap_halves(
                acts_ref[2 * pair, k].astype(jnp.float32), acts_ref[2 * pair + 1, k].astype(jnp.float32)
            )
            stack[upper, lanes] = first.astype(stack.dtype)
            stack[lower, lanes] = second.astype(stack.dtype)
        return carry

    lax.fori_loop(0, pieces, unpack, 0)

    below = lax.broadcasted_iota(jnp.int32, (TILE, TILE), 1) <= lax.broadcasted_iota(jnp.int32, (TILE, TILE), 0)
    row8 = lax.broadcasted_iota(jnp.int32, (8, TILE), 0)
    bias_rows = jnp.zeros((8, TILE), jnp.float32)
    zero = jnp.zeros((TILE, TILE), jnp.bfloat16)
    for d in range(8):
        slot = lax.rem(quad - d // 2 + 4, 4)
        mine = core == d % 2

        def held(first, count):
            rows = pl.ds(first, count)
            return jnp.where(mine, own_ref[slot, rows, :].astype(jnp.float32), other_ref[slot, rows, :].astype(jnp.float32))

        for b in range(5):
            if b <= d:
                q, p = d, b
            elif b >= d + 2:
                q, p = 7 - d, 9 - b
            else:
                continue
            block = held(b * TILE, TILE)
            if p == q:
                block = jnp.where(below, block, 0.0)
            weight[q * TILE : (q + 1) * TILE, p * TILE : (p + 1) * TILE] = block.astype(jnp.bfloat16)
        if d % 2 == 0:
            weight[d * TILE : (d + 1) * TILE, (d + 1) * TILE : (d + 2) * TILE] = zero
        pair = held(5 * TILE, 16)
        bias = pair[0:1, :] + pair[1:2, :]
        bias_rows = jnp.where(row8 == d, bias, bias_rows)
    bias_columns = bias_rows.T

    def block_of(n, carry):
        base = n * SPAN
        for i in (3, 2, 1, 0):
            depth = (i + 1) * 256
            summed = jnp.dot(
                weight[i * 256 : (i + 1) * 256, :depth],
                stack[pl.ds(pl.multiple_of(base, SPAN), depth), :],
                preferred_element_type=jnp.float32,
            )
            for h in range(2):
                d = 2 * i + h
                mixed = summed[h * TILE : (h + 1) * TILE] + bias_columns[:, d : d + 1]
                stack[pl.ds(pl.multiple_of(base + d * TILE, TILE), TILE), :] = mixed.astype(stack.dtype)
        return carry

    lax.fori_loop(0, pieces * 2 * half // SPAN, block_of, 0)

    def repack(k, carry):
        upper = pl.ds(pl.multiple_of(k * 2 * half, 2 * half), half)
        lower = pl.ds(pl.multiple_of(k * 2 * half + half, half), half)
        for pair in range(2):
            lanes = pl.ds(pair * TILE, TILE)
            first, second = swap_halves(stack[upper, lanes].astype(jnp.float32), stack[lower, lanes].astype(jnp.float32))
            out_ref[2 * pair, k] = first.astype(out_ref.dtype)
            out_ref[2 * pair + 1, k] = second.astype(out_ref.dtype)
        return carry

    lax.fori_loop(0, pieces, repack, 0)


def gate_kernel(gate_ref, mixed_ref, out_ref):
    rows, channels = gate_ref.shape
    half = rows // 2
    step = 16

    def chunk(i, carry):
        top = pl.ds(pl.multiple_of(i * step, step), step)
        bottom = pl.ds(pl.multiple_of(half + i * step, step), step)
        for t in range(channels // TILE):
            lanes = pl.ds(t * TILE, TILE)
            upper, lower = swap_halves(
                mixed_ref[2 * t, top, :].astype(jnp.float32), mixed_ref[2 * t + 1, top, :].astype(jnp.float32)
            )
            for place, mixed in ((top, upper), (bottom, lower)):
                act = jax.nn.gelu(gate_ref[place, lanes].astype(jnp.float32))
                out_ref[place, lanes] = (act * mixed).astype(out_ref.dtype)
        return carry

    lax.fori_loop(0, half // step, chunk, 0)


def call(kernel, name, out_shape, specs, flops, moved, scratch=()):
    return pl.pallas_call(
        kernel,
        name=name,
        out_shape=jax.ShapeDtypeStruct(out_shape, jnp.bfloat16),
        in_specs=specs,
        out_specs=VMEM,
        scratch_shapes=list(scratch),
        cost_estimate=pl.CostEstimate(flops=flops, bytes_accessed=moved, transcendentals=0),
    )


def local(gate_input, value_input, norm_gain, norm_bias, mix_weight, mix_bias):
    _, rows, channels = value_input.shape
    groups = channels // GROUP_DIM
    half = rows // 2
    x, core, quad = lax.axis_index("x"), lax.axis_index("core"), lax.axis_index("zq")

    weight = mix_weight[0]
    excess = lax.ppermute(weight[:, 5 * TILE :], ("x", "core"), [(5, 2), (6, 1), (7, 0)])
    place = jnp.stack([2 * x + core]).astype(jnp.int32)
    folded = call(fold_kernel, "fold", (5 * TILE + 16, TILE), [SMEM, VMEM, VMEM, VMEM], 1000000, 600000)(
        place, weight, excess, mix_bias.reshape(SPAN // TILE, TILE)
    )
    received = []
    for k in range(4):
        pairs = [(z * 4 + s, ((s + k) % 4) * 4 + z) for z in range(4) for s in range(4)]
        received.append(lax.ppermute(folded, ("zq", "x"), pairs))
    own = jnp.stack(received)
    other = lax.ppermute(own, "core", [(0, 1), (1, 0)])

    normed = call(
        norm_kernel,
        "norm",
        (groups, half, TILE),
        [VMEM, VMEM, VMEM],
        40000000,
        3200000,
        [pltpu.VMEM((32, channels), jnp.float32)],
    )(value_input[0], norm_gain.reshape(1, channels), norm_bias.reshape(1, channels))
    acts = lax.all_to_all(normed, QUAD, split_axis=0, concat_axis=0, tiled=True)

    mixed = call(
        mix_kernel,
        "mix",
        (4, groups // 4, half, TILE),
        [SMEM, VMEM, VMEM, VMEM],
        1000000000,
        6000000,
        [pltpu.VMEM((SPAN, SPAN), jnp.bfloat16), pltpu.VMEM((groups // 4 * rows, 2 * TILE), jnp.bfloat16)],
    )(jnp.stack([quad, core]).astype(jnp.int32), acts.reshape(4, groups // 4, half, TILE), own, other)
    returned = lax.all_to_all(mixed.reshape(groups, half, TILE), QUAD, split_axis=0, concat_axis=0, tiled=True)

    gated = call(gate_kernel, "gate", (rows, channels), [VMEM, VMEM], 40000000, 4800000)(gate_input[0], returned)
    return gated[None]


def solution(mesh):
    devices = mesh.devices.reshape(4, 4, 4, 4, 2)
    split = Mesh(devices, ("zq", "zr", "y", "x", "core"))
    sp, dp = ("zq", "zr", "y"), ("x", "core")
    in_specs = (P(dp, sp, None), P(dp, sp, None), P(), P(), P(sp, dp, None), P(sp, None))
    return jax.shard_map(local, mesh=split, in_specs=in_specs, out_specs=P(dp, sp, None), check_vma=False)
```

```python
import jax
import jax.numpy as jnp
from jax import lax
from jax.experimental import pallas as pl
from jax.experimental.pallas import tpu as pltpu
from jax.sharding import Mesh
from jax.sharding import PartitionSpec as P

GROUP_DIM = 64
SPAN = 1024
TILE = 128
EPSILON = 1e-05
QUAD = ("x", "zr", "y")

VMEM = pl.BlockSpec(memory_space=pltpu.VMEM)
SMEM = pl.BlockSpec(memory_space=pltpu.SMEM)
HBM = pl.BlockSpec(memory_space=pltpu.HBM)


def lane_is_low(shape):
    return lax.broadcasted_iota(jnp.int32, shape, 1) < GROUP_DIM


def swap_halves(upper, lower):
    low = lane_is_low(upper.shape)
    first = jnp.where(low, upper, pltpu.roll(lower, GROUP_DIM, 1))
    second = jnp.where(low, pltpu.roll(upper, GROUP_DIM, 1), lower)
    return first, second


STEP = 16


def row_pieces(rows):
    half = rows // 2
    return [(side, i) for i in range(half // STEP) for side in range(2)]


def fetch(source_ref, target_ref, sems, side, i):
    place = pl.ds(side * (source_ref.shape[0] // 2) + i * STEP, STEP)
    return pltpu.make_async_copy(source_ref.at[place], target_ref.at[place], sems.at[side, i])


def norm_kernel(value_hbm, gain_ref, bias_ref, out_ref, act_ref, value_ref, sems):
    rows, channels = value_hbm.shape
    half = rows // 2
    step = STEP
    tiles = channels // TILE
    for side, i in row_pieces(rows):
        fetch(value_hbm, value_ref, sems, side, i).start()

    def chunk(i, carry):
        top = pl.ds(pl.multiple_of(i * step, step), step)
        bottom = pl.ds(pl.multiple_of(half + i * step, step), step)
        for side in range(2):
            fetch(value_hbm, value_ref, sems, side, i).wait()
        total = jnp.zeros((2 * step, TILE), jnp.float32)
        for t in range(tiles):
            lanes = pl.ds(t * TILE, TILE)
            both = jnp.concatenate([value_ref[top, lanes], value_ref[bottom, lanes]], axis=0)
            act = jax.nn.gelu(both.astype(jnp.float32))
            act_ref[:, lanes] = act
            total = total + act
        centre = jnp.sum(total, axis=1, keepdims=True) * (1.0 / channels)
        square = jnp.zeros((2 * step, TILE), jnp.float32)
        for t in range(tiles):
            shifted = act_ref[:, pl.ds(t * TILE, TILE)] - centre
            square = square + shifted * shifted
        variance = jnp.sum(square, axis=1, keepdims=True) * (1.0 / channels)
        scale = lax.rsqrt(variance + EPSILON)
        for t in range(tiles):
            lanes = pl.ds(t * TILE, TILE)
            shifted = act_ref[:, lanes] - centre
            normed = shifted * scale * gain_ref[:, lanes] + bias_ref[:, lanes]
            first, second = swap_halves(normed[:step], normed[step:])
            out_ref[2 * t, top, :] = first.astype(out_ref.dtype)
            out_ref[2 * t + 1, top, :] = second.astype(out_ref.dtype)
        return carry

    lax.fori_loop(0, half // step, chunk, 0)


def fold_kernel(place_ref, weight_ref, excess_ref, bias_ref, out_ref):
    d = place_ref[0]
    for b in range(5):
        block = weight_ref[:, b * TILE : (b + 1) * TILE]
        if b >= 2:
            e = 4 - b
            block = jnp.where(b >= d + 2, excess_ref[:, e * TILE : (e + 1) * TILE], block)
        out_ref[b * TILE : (b + 1) * TILE, :] = block
    bias = bias_ref[pl.ds(d, 1), :]
    high = bias.astype(jnp.bfloat16).astype(jnp.float32)
    low = bias - high
    row = lax.broadcasted_iota(jnp.int32, (16, TILE), 0)
    pair = jnp.where(row == 0, high, jnp.where(row == 1, low, 0.0))
    out_ref[5 * TILE :, :] = pair.astype(out_ref.dtype)


def mix_kernel(place_ref, acts_ref, own_ref, other_ref, out_ref, weight, stack):
    column_of_x, core = place_ref[0], place_ref[1]
    pieces, half, _ = acts_ref.shape[1:]

    def unpack(k, carry):
        upper = pl.ds(pl.multiple_of(k * 2 * half, 2 * half), half)
        lower = pl.ds(pl.multiple_of(k * 2 * half + half, half), half)
        for pair in range(2):
            lanes = pl.ds(pair * TILE, TILE)
            first, second = swap_halves(
                acts_ref[2 * pair, k].astype(jnp.float32), acts_ref[2 * pair + 1, k].astype(jnp.float32)
            )
            stack[upper, lanes] = first.astype(stack.dtype)
            stack[lower, lanes] = second.astype(stack.dtype)
        return carry

    lax.fori_loop(0, pieces, unpack, 0)

    below = lax.broadcasted_iota(jnp.int32, (TILE, TILE), 1) <= lax.broadcasted_iota(jnp.int32, (TILE, TILE), 0)
    row8 = lax.broadcasted_iota(jnp.int32, (8, TILE), 0)
    bias_rows = jnp.zeros((8, TILE), jnp.float32)
    zero = jnp.zeros((TILE, TILE), jnp.bfloat16)
    for d in range(8):
        slot = lax.rem(column_of_x - d // 2 + 4, 4)
        mine = core == d % 2

        def held(first, count):
            rows = pl.ds(first, count)
            return jnp.where(mine, own_ref[slot, rows, :].astype(jnp.float32), other_ref[slot, rows, :].astype(jnp.float32))

        for b in range(5):
            if b <= d:
                q, p = d, b
            elif b >= d + 2:
                q, p = 7 - d, 9 - b
            else:
                continue
            block = held(b * TILE, TILE)
            if p == q:
                block = jnp.where(below, block, 0.0)
            weight[q * TILE : (q + 1) * TILE, p * TILE : (p + 1) * TILE] = block.astype(jnp.bfloat16)
        for p in range(d + 1, d // 4 * 4 + 4):
            weight[d * TILE : (d + 1) * TILE, p * TILE : (p + 1) * TILE] = zero
        pair = held(5 * TILE, 16)
        bias = pair[0:1, :] + pair[1:2, :]
        bias_rows = jnp.where(row8 == d, bias, bias_rows)
    bias_columns = bias_rows.T

    def block_of(n, carry):
        base = n * SPAN
        for i in (1, 0):
            depth = (i + 1) * 512
            summed = jnp.dot(
                weight[i * 512 : (i + 1) * 512, :depth],
                stack[pl.ds(pl.multiple_of(base, SPAN), depth), :],
                preferred_element_type=jnp.float32,
            )
            for h in range(4):
                d = 4 * i + h
                mixed = summed[h * TILE : (h + 1) * TILE] + bias_columns[:, d : d + 1]
                stack[pl.ds(pl.multiple_of(base + d * TILE, TILE), TILE), :] = mixed.astype(stack.dtype)
        return carry

    lax.fori_loop(0, pieces * 2 * half // SPAN, block_of, 0)

    def repack(k, carry):
        upper = pl.ds(pl.multiple_of(k * 2 * half, 2 * half), half)
        lower = pl.ds(pl.multiple_of(k * 2 * half + half, half), half)
        for pair in range(2):
            lanes = pl.ds(pair * TILE, TILE)
            first, second = swap_halves(stack[upper, lanes].astype(jnp.float32), stack[lower, lanes].astype(jnp.float32))
            out_ref[2 * pair, k] = first.astype(out_ref.dtype)
            out_ref[2 * pair + 1, k] = second.astype(out_ref.dtype)
        return carry

    lax.fori_loop(0, pieces, repack, 0)


def gate_kernel(gate_ref, mixed_ref, out_hbm, out_ref, out_sems):
    rows, channels = gate_ref.shape
    half = rows // 2
    step = STEP

    def send(side, i):
        place = pl.ds(side * half + i * step, step)
        return pltpu.make_async_copy(out_ref.at[place], out_hbm.at[place], out_sems.at[side, i])

    def chunk(i, carry):
        top = pl.ds(pl.multiple_of(i * step, step), step)
        bottom = pl.ds(pl.multiple_of(half + i * step, step), step)
        for t in range(channels // TILE):
            lanes = pl.ds(t * TILE, TILE)
            upper, lower = swap_halves(
                mixed_ref[2 * t, top, :].astype(jnp.float32), mixed_ref[2 * t + 1, top, :].astype(jnp.float32)
            )
            for place, mixed in ((top, upper), (bottom, lower)):
                act = jax.nn.gelu(gate_ref[place, lanes].astype(jnp.float32))
                out_ref[place, lanes] = (act * mixed).astype(out_ref.dtype)
        for side in range(2):
            send(side, i).start()
        return carry

    lax.fori_loop(0, half // step, chunk, 0)
    for side, i in row_pieces(rows):
        send(side, i).wait()


def call(kernel, out_shape, specs, flops, moved, scratch=(), out_spec=VMEM, limit=16):
    if out_spec is VMEM:
        out = pltpu.VMEM(out_shape, jnp.bfloat16)
    else:
        out = jax.ShapeDtypeStruct(out_shape, jnp.bfloat16)
    return pl.pallas_call(
        kernel,
        out_shape=out,
        in_specs=specs,
        out_specs=out_spec,
        scratch_shapes=list(scratch),
        cost_estimate=pl.CostEstimate(flops=flops, bytes_accessed=moved, transcendentals=0),
        compiler_params=pltpu.CompilerParams(vmem_limit_bytes=limit << 20),
    )


def near(array):
    return pltpu.with_memory_space_constraint(array, pltpu.VMEM)


def copy_slots(rows):
    return pltpu.SemaphoreType.DMA((2, rows // 2 // STEP))


def local(gate_input, value_input, norm_gain, norm_bias, mix_weight, mix_bias):
    _, rows, channels = value_input.shape
    groups = channels // GROUP_DIM
    half = rows // 2
    x, core = lax.axis_index("x"), lax.axis_index("core")

    weight = mix_weight[0]
    excess = lax.ppermute(weight[:, 5 * TILE :], ("x", "core"), [(5, 2), (6, 1), (7, 0)])
    place = jnp.stack([2 * x + core]).astype(jnp.int32)
    folded = call(fold_kernel, (5 * TILE + 16, TILE), [SMEM, VMEM, VMEM, VMEM], 1000000, 600000)(
        place, weight, excess, mix_bias.reshape(SPAN // TILE, TILE)
    )
    quads = lax.all_gather(folded, "zq", axis=0)
    normed = call(
        norm_kernel,
        (groups, half, TILE),
        [HBM, VMEM, VMEM],
        40000000,
        3200000,
        [pltpu.VMEM((32, channels), jnp.float32), pltpu.VMEM((rows, channels), jnp.bfloat16), copy_slots(rows)],
        limit=60,
    )(value_input[0], norm_gain.reshape(1, channels), norm_bias.reshape(1, channels))
    normed, quads = lax.optimization_barrier((normed, quads))
    acts = lax.all_to_all(normed, QUAD, split_axis=0, concat_axis=0, tiled=True)

    received = []
    for s in range(4):
        piece = lax.dynamic_index_in_dim(quads, lax.rem(x + s, 4), 0, keepdims=False)
        received.append(lax.ppermute(piece, "x", [(i, (i + s) % 4) for i in range(4)]) if s else piece)
    own = jnp.stack(received)
    other = lax.ppermute(own, "core", [(0, 1), (1, 0)])

    mixed = call(
        mix_kernel,
        (4, groups // 4, half, TILE),
        [SMEM, VMEM, VMEM, VMEM],
        1000000000,
        6000000,
        [pltpu.VMEM((SPAN, SPAN), jnp.bfloat16), pltpu.VMEM((groups // 4 * rows, 2 * TILE), jnp.bfloat16)],
    )(jnp.stack([x, core]).astype(jnp.int32), near(acts.reshape(4, groups // 4, half, TILE)), near(own), near(other))
    returned = lax.all_to_all(mixed.reshape(groups, half, TILE), QUAD, split_axis=0, concat_axis=0, tiled=True)

    gated = call(
        gate_kernel,
        (rows, channels),
        [VMEM, VMEM],
        40000000,
        4800000,
        [pltpu.VMEM((rows, channels), jnp.bfloat16), copy_slots(rows)],
        HBM,
    )(near(gate_input[0]), near(returned))
    return gated[None]


def solution(mesh):
    devices = mesh.devices.reshape(4, 4, 4, 4, 2)
    split = Mesh(devices, ("zq", "zr", "y", "x", "core"))
    sp, dp = ("zq", "zr", "y"), ("x", "core")
    in_specs = (P(dp, sp, None), P(dp, sp, None), P(), P(), P(sp, dp, None), P(sp, None))
    return jax.shard_map(local, mesh=split, in_specs=in_specs, out_specs=P(dp, sp, None), check_vma=False)
```

```python
import jax
import jax.numpy as jnp
from jax import lax
from jax.experimental import pallas as pl
from jax.experimental.pallas import tpu as pltpu
from jax.sharding import Mesh
from jax.sharding import PartitionSpec as P

GROUP_DIM = 64
SPAN = 1024
TILE = 128
EPSILON = 1e-05
HALF = TILE // 2
HALVES = 9
QUAD = ("x", "zr", "y")

VMEM = pl.BlockSpec(memory_space=pltpu.VMEM)
SMEM = pl.BlockSpec(memory_space=pltpu.SMEM)
HBM = pl.BlockSpec(memory_space=pltpu.HBM)


def lane_is_low(shape):
    return lax.broadcasted_iota(jnp.int32, shape, 1) < GROUP_DIM


def swap_halves(upper, lower):
    low = lane_is_low(upper.shape)
    first = jnp.where(low, upper, pltpu.roll(lower, GROUP_DIM, 1))
    second = jnp.where(low, pltpu.roll(upper, GROUP_DIM, 1), lower)
    return first, second


STEP = 16


def row_pieces(rows):
    half = rows // 2
    return [(side, i) for i in range(half // STEP) for side in range(2)]


def fetch(source_ref, target_ref, sems, side, i):
    place = pl.ds(side * (source_ref.shape[0] // 2) + i * STEP, STEP)
    return pltpu.make_async_copy(source_ref.at[place], target_ref.at[place], sems.at[side, i])


def norm_kernel(value_hbm, gain_ref, bias_ref, out_ref, act_ref, value_ref, sems):
    rows, channels = value_hbm.shape
    half = rows // 2
    step = STEP
    tiles = channels // TILE
    for side, i in row_pieces(rows):
        fetch(value_hbm, value_ref, sems, side, i).start()

    def chunk(i, carry):
        top = pl.ds(pl.multiple_of(i * step, step), step)
        bottom = pl.ds(pl.multiple_of(half + i * step, step), step)
        for side in range(2):
            fetch(value_hbm, value_ref, sems, side, i).wait()
        total = jnp.zeros((2 * step, TILE), jnp.float32)
        for t in range(tiles):
            lanes = pl.ds(t * TILE, TILE)
            both = jnp.concatenate([value_ref[top, lanes], value_ref[bottom, lanes]], axis=0)
            act = jax.nn.gelu(both.astype(jnp.float32))
            act_ref[:, lanes] = act
            total = total + act
        centre = jnp.sum(total, axis=1, keepdims=True) * (1.0 / channels)
        square = jnp.zeros((2 * step, TILE), jnp.float32)
        for t in range(tiles):
            shifted = act_ref[:, pl.ds(t * TILE, TILE)] - centre
            square = square + shifted * shifted
        variance = jnp.sum(square, axis=1, keepdims=True) * (1.0 / channels)
        scale = lax.rsqrt(variance + EPSILON)
        for t in range(tiles):
            lanes = pl.ds(t * TILE, TILE)
            shifted = act_ref[:, lanes] - centre
            normed = shifted * scale * gain_ref[:, lanes] + bias_ref[:, lanes]
            first, second = swap_halves(normed[:step], normed[step:])
            out_ref[2 * t, top, :] = first.astype(out_ref.dtype)
            out_ref[2 * t + 1, top, :] = second.astype(out_ref.dtype)
        return carry

    lax.fori_loop(0, half // step, chunk, 0)


def half_of(ref, h):
    return ref[h % 2 * HALF : (h % 2 + 1) * HALF, h // 2 * TILE : (h // 2 + 1) * TILE]


def fold_kernel(place_ref, weight_ref, excess_ref, bias_ref, out_ref):
    d = place_ref[0]
    for h in range(HALVES):
        block = half_of(weight_ref, h)
        if h >= 2:
            moved = half_of(excess_ref, 2 * HALVES - 1 - h - 8)
            block = jnp.where(h >= 2 * d + 2, moved, block)
        out_ref[h * HALF : (h + 1) * HALF, :] = block
    bias = bias_ref[pl.ds(d, 1), :]
    high = bias.astype(jnp.bfloat16).astype(jnp.float32)
    low = bias - high
    row = lax.broadcasted_iota(jnp.int32, (16, TILE), 0)
    pair = jnp.where(row == 0, high, jnp.where(row == 1, low, 0.0))
    out_ref[HALVES * HALF :, :] = pair.astype(out_ref.dtype)


def unfold_kernel(place_ref, own_ref, other_ref, weight, bias_ref):
    column_of_x, core = place_ref[0], place_ref[1]
    row8 = lax.broadcasted_iota(jnp.int32, (8, TILE), 0)
    column = lax.broadcasted_iota(jnp.int32, (HALF, TILE), 1)
    line = lax.broadcasted_iota(jnp.int32, (HALF, TILE), 0)
    bias_rows = jnp.zeros((8, TILE), jnp.float32)
    zero = jnp.zeros((TILE, TILE), jnp.bfloat16)
    for d in range(8):
        slot = lax.rem(column_of_x - d // 2 + 4, 4)
        mine = core == d % 2

        def held(first, count):
            rows = pl.ds(first, count)
            return jnp.where(mine, own_ref[slot, rows, :].astype(jnp.float32), other_ref[slot, rows, :].astype(jnp.float32))

        for h in range(HALVES):
            block = held(h * HALF, HALF)
            q, place = (d, h) if h <= 2 * d + 1 else (7 - d, 2 * HALVES - 1 - h)
            p, side = place // 2, place % 2
            if p == q:
                block = jnp.where(column <= line + side * HALF, block, 0.0)
            first = q * TILE + side * HALF
            weight[first : first + HALF, p * TILE : (p + 1) * TILE] = block.astype(jnp.bfloat16)
        for p in range(d + 1, d // 4 * 4 + 4):
            weight[d * TILE : (d + 1) * TILE, p * TILE : (p + 1) * TILE] = zero
        pair = held(HALVES * HALF, 16)
        bias = pair[0:1, :] + pair[1:2, :]
        bias_rows = jnp.where(row8 == d, bias, bias_rows)
    bias_ref[...] = bias_rows


def mix_kernel(acts_ref, weight_hbm, bias_ref, out_ref, weight, stack, sem):
    pieces, half, _ = acts_ref.shape[1:]
    weight_copy = pltpu.make_async_copy(weight_hbm, weight, sem)
    weight_copy.start()

    def unpack(k, carry):
        upper = pl.ds(pl.multiple_of(k * 2 * half, 2 * half), half)
        lower = pl.ds(pl.multiple_of(k * 2 * half + half, half), half)
        for pair in range(2):
            lanes = pl.ds(pair * TILE, TILE)
            first, second = swap_halves(
                acts_ref[2 * pair, k].astype(jnp.float32), acts_ref[2 * pair + 1, k].astype(jnp.float32)
            )
            stack[upper, lanes] = first.astype(stack.dtype)
            stack[lower, lanes] = second.astype(stack.dtype)
        return carry

    lax.fori_loop(0, pieces, unpack, 0, unroll=True)

    bias_columns = bias_ref[...].T

    weight_copy.wait()
    for n in range(pieces * 2 * half // SPAN):
        base = n * SPAN
        for i in (1, 0):
            depth = (i + 1) * 512
            summed = jnp.dot(
                weight[i * 512 : (i + 1) * 512, :depth],
                stack[base : base + depth, :],
                preferred_element_type=jnp.float32,
            )
            for h in range(4):
                d = 4 * i + h
                mixed = summed[h * TILE : (h + 1) * TILE] + bias_columns[:, d : d + 1]
                stack[base + d * TILE : base + (d + 1) * TILE, :] = mixed.astype(stack.dtype)

    def repack(k, carry):
        upper = pl.ds(pl.multiple_of(k * 2 * half, 2 * half), half)
        lower = pl.ds(pl.multiple_of(k * 2 * half + half, half), half)
        for pair in range(2):
            lanes = pl.ds(pair * TILE, TILE)
            first, second = swap_halves(stack[upper, lanes].astype(jnp.float32), stack[lower, lanes].astype(jnp.float32))
            out_ref[2 * pair, k] = first.astype(out_ref.dtype)
            out_ref[2 * pair + 1, k] = second.astype(out_ref.dtype)
        return carry

    lax.fori_loop(0, pieces, repack, 0, unroll=True)


def gate_kernel(gate_ref, mixed_ref, out_hbm, out_ref, out_sems):
    rows, channels = gate_ref.shape
    half = rows // 2
    step = STEP

    def send(side, i):
        place = pl.ds(side * half + i * step, step)
        return pltpu.make_async_copy(out_ref.at[place], out_hbm.at[place], out_sems.at[side, i])

    def chunk(i, carry):
        top = pl.ds(pl.multiple_of(i * step, step), step)
        bottom = pl.ds(pl.multiple_of(half + i * step, step), step)
        for t in range(channels // TILE):
            lanes = pl.ds(t * TILE, TILE)
            upper, lower = swap_halves(
                mixed_ref[2 * t, top, :].astype(jnp.float32), mixed_ref[2 * t + 1, top, :].astype(jnp.float32)
            )
            for place, mixed in ((top, upper), (bottom, lower)):
                act = jax.nn.gelu(gate_ref[place, lanes].astype(jnp.float32))
                out_ref[place, lanes] = (act * mixed).astype(out_ref.dtype)
        for side in range(2):
            send(side, i).start()
        return carry

    lax.fori_loop(0, half // step, chunk, 0)
    for side, i in row_pieces(rows):
        send(side, i).wait()


def call(kernel, out_shape, specs, flops, moved, scratch=(), out_spec=VMEM, limit=16):
    if out_spec is VMEM:
        out = pltpu.VMEM(out_shape, jnp.bfloat16)
    else:
        out = jax.ShapeDtypeStruct(out_shape, jnp.bfloat16)
    return pl.pallas_call(
        kernel,
        out_shape=out,
        in_specs=specs,
        out_specs=out_spec,
        scratch_shapes=list(scratch),
        cost_estimate=pl.CostEstimate(flops=flops, bytes_accessed=moved, transcendentals=0),
        compiler_params=pltpu.CompilerParams(vmem_limit_bytes=limit << 20),
    )


def near(array):
    return pltpu.with_memory_space_constraint(array, pltpu.VMEM)


def copy_slots(rows):
    return pltpu.SemaphoreType.DMA((2, rows // 2 // STEP))


def local(gate_input, value_input, norm_gain, norm_bias, mix_weight, mix_bias):
    _, rows, channels = value_input.shape
    groups = channels // GROUP_DIM
    half = rows // 2
    x, core = lax.axis_index("x"), lax.axis_index("core")

    weight = mix_weight[0]
    excess = lax.ppermute(weight[:, 4 * TILE :], ("x", "core"), [(4, 3), (5, 2), (6, 1), (7, 0)])
    place = jnp.stack([2 * x + core]).astype(jnp.int32)
    folded = call(fold_kernel, (HALVES * HALF + 16, TILE), [SMEM, VMEM, VMEM, VMEM], 1000000, 600000)(
        place, weight, excess, mix_bias.reshape(SPAN // TILE, TILE)
    )
    quads = lax.all_gather(folded, "zq", axis=0)
    normed = call(
        norm_kernel,
        (groups, half, TILE),
        [HBM, VMEM, VMEM],
        40000000,
        3200000,
        [pltpu.VMEM((32, channels), jnp.float32), pltpu.VMEM((rows, channels), jnp.bfloat16), copy_slots(rows)],
        limit=60,
    )(value_input[0], norm_gain.reshape(1, channels), norm_bias.reshape(1, channels))
    normed, quads = lax.optimization_barrier((normed, quads))
    acts = lax.all_to_all(normed, QUAD, split_axis=0, concat_axis=0, tiled=True)

    received = []
    for s in range(4):
        piece = lax.dynamic_index_in_dim(quads, lax.rem(x + s, 4), 0, keepdims=False)
        received.append(lax.ppermute(piece, "x", [(i, (i + s) % 4) for i in range(4)]) if s else piece)
    own = jnp.stack(received)
    other = lax.ppermute(own, "core", [(0, 1), (1, 0)])

    full, bias_rows = pl.pallas_call(
        unfold_kernel,
        name="unfold",
        out_shape=(jax.ShapeDtypeStruct((SPAN, SPAN), jnp.bfloat16), pltpu.VMEM((8, TILE), jnp.float32)),
        in_specs=[SMEM, VMEM, VMEM],
        out_specs=(VMEM, VMEM),
        cost_estimate=pl.CostEstimate(flops=5000000, bytes_accessed=4000000, transcendentals=0),
        compiler_params=pltpu.CompilerParams(vmem_limit_bytes=16 << 20),
    )(jnp.stack([x, core]).astype(jnp.int32), near(own), near(other))
    mixed = call(
        mix_kernel,
        (4, groups // 4, half, TILE),
        [VMEM, HBM, VMEM],
        1000000000,
        6000000,
        [
            pltpu.VMEM((SPAN, SPAN), jnp.bfloat16),
            pltpu.VMEM((groups // 4 * rows, 2 * TILE), jnp.bfloat16),
            pltpu.SemaphoreType.DMA(()),
        ],
    )(near(acts.reshape(4, groups // 4, half, TILE)), pltpu.with_memory_space_constraint(full, pltpu.HBM), near(bias_rows))
    returned = lax.all_to_all(mixed.reshape(groups, half, TILE), QUAD, split_axis=0, concat_axis=0, tiled=True)

    gated = call(
        gate_kernel,
        (rows, channels),
        [VMEM, VMEM],
        40000000,
        4800000,
        [pltpu.VMEM((rows, channels), jnp.bfloat16), copy_slots(rows)],
        HBM,
    )(near(gate_input[0]), near(returned))
    return gated[None]


def solution(mesh):
    devices = mesh.devices.reshape(4, 4, 4, 4, 2)
    split = Mesh(devices, ("zq", "zr", "y", "x", "core"))
    sp, dp = ("zq", "zr", "y"), ("x", "core")
    in_specs = (P(dp, sp, None), P(dp, sp, None), P(), P(), P(sp, dp, None), P(sp, None))
    return jax.shard_map(local, mesh=split, in_specs=in_specs, out_specs=P(dp, sp, None), check_vma=False)
```

```python
import jax
import jax.numpy as jnp
from jax import lax
from jax.experimental import pallas as pl
from jax.experimental.pallas import tpu as pltpu
from jax.sharding import Mesh
from jax.sharding import PartitionSpec as P

GROUP_DIM = 64
SPAN = 1024
TILE = 128
EPSILON = 1e-05
HALF = TILE // 2
HALVES = 9
QUAD = ("x", "zr", "y")

VMEM = pl.BlockSpec(memory_space=pltpu.VMEM)
SMEM = pl.BlockSpec(memory_space=pltpu.SMEM)
HBM = pl.BlockSpec(memory_space=pltpu.HBM)


def lane_is_low(shape):
    return lax.broadcasted_iota(jnp.int32, shape, 1) < GROUP_DIM


def swap_halves(upper, lower):
    low = lane_is_low(upper.shape)
    first = jnp.where(low, upper, pltpu.roll(lower, GROUP_DIM, 1))
    second = jnp.where(low, pltpu.roll(upper, GROUP_DIM, 1), lower)
    return first, second


STEP = 32


def row_pieces(rows):
    half = rows // 2
    return [(side, i) for i in range(half // STEP) for side in range(2)]


def norm_kernel(value_ref, gain_ref, bias_ref, out_ref, act_ref):
    rows, channels = value_ref.shape
    half = rows // 2
    step = 32
    tiles = channels // TILE

    def chunk(i, carry):
        top = pl.ds(pl.multiple_of(i * step, step), step)
        bottom = pl.ds(pl.multiple_of(half + i * step, step), step)
        total = jnp.zeros((2 * step, TILE), jnp.float32)
        for t in range(tiles):
            lanes = pl.ds(t * TILE, TILE)
            both = jnp.concatenate([value_ref[top, lanes], value_ref[bottom, lanes]], axis=0)
            act = jax.nn.gelu(both.astype(jnp.float32))
            act_ref[:, lanes] = act
            total = total + act
        centre = jnp.sum(total, axis=1, keepdims=True) * (1.0 / channels)
        square = jnp.zeros((2 * step, TILE), jnp.float32)
        for t in range(tiles):
            shifted = act_ref[:, pl.ds(t * TILE, TILE)] - centre
            square = square + shifted * shifted
        variance = jnp.sum(square, axis=1, keepdims=True) * (1.0 / channels)
        scale = lax.rsqrt(variance + EPSILON)
        for t in range(tiles):
            lanes = pl.ds(t * TILE, TILE)
            shifted = act_ref[:, lanes] - centre
            normed = shifted * scale * gain_ref[:, lanes] + bias_ref[:, lanes]
            first, second = swap_halves(normed[:step], normed[step:])
            out_ref[2 * t, top, :] = first.astype(out_ref.dtype)
            out_ref[2 * t + 1, top, :] = second.astype(out_ref.dtype)
        return carry

    lax.fori_loop(0, half // step, chunk, 0)


def half_of(ref, h):
    return ref[h % 2 * HALF : (h % 2 + 1) * HALF, h // 2 * TILE : (h // 2 + 1) * TILE]


def fold_kernel(place_ref, weight_ref, excess_ref, bias_ref, out_ref):
    d = place_ref[0]
    for h in range(HALVES):
        block = half_of(weight_ref, h)
        if h >= 2:
            moved = half_of(excess_ref, 2 * HALVES - 1 - h - 8)
            block = jnp.where(h >= 2 * d + 2, moved, block)
        out_ref[h * HALF : (h + 1) * HALF, :] = block
    bias = bias_ref[pl.ds(d, 1), :]
    high = bias.astype(jnp.bfloat16).astype(jnp.float32)
    low = bias - high
    row = lax.broadcasted_iota(jnp.int32, (16, TILE), 0)
    pair = jnp.where(row == 0, high, jnp.where(row == 1, low, 0.0))
    out_ref[HALVES * HALF :, :] = pair.astype(out_ref.dtype)


def unfold_kernel(place_ref, own_ref, other_ref, weight, bias_ref):
    column_of_x, core = place_ref[0], place_ref[1]
    row8 = lax.broadcasted_iota(jnp.int32, (8, TILE), 0)
    column = lax.broadcasted_iota(jnp.int32, (HALF, TILE), 1)
    line = lax.broadcasted_iota(jnp.int32, (HALF, TILE), 0)
    bias_rows = jnp.zeros((8, TILE), jnp.float32)
    zero = jnp.zeros((TILE, TILE), jnp.bfloat16)
    for d in range(8):
        slot = lax.rem(column_of_x - d // 2 + 4, 4)
        mine = core == d % 2

        def held(first, count):
            rows = pl.ds(first, count)
            return jnp.where(mine, own_ref[slot, rows, :].astype(jnp.float32), other_ref[slot, rows, :].astype(jnp.float32))

        for h in range(HALVES):
            block = held(h * HALF, HALF)
            q, place = (d, h) if h <= 2 * d + 1 else (7 - d, 2 * HALVES - 1 - h)
            p, side = place // 2, place % 2
            if p == q:
                block = jnp.where(column <= line + side * HALF, block, 0.0)
            first = q * TILE + side * HALF
            weight[first : first + HALF, p * TILE : (p + 1) * TILE] = block.astype(jnp.bfloat16)
        for p in range(d + 1, d // 4 * 4 + 4):
            weight[d * TILE : (d + 1) * TILE, p * TILE : (p + 1) * TILE] = zero
        pair = held(HALVES * HALF, 16)
        bias = pair[0:1, :] + pair[1:2, :]
        bias_rows = jnp.where(row8 == d, bias, bias_rows)
    bias_ref[...] = bias_rows


def mix_kernel(acts_ref, weight_hbm, bias_ref, out_ref, weight, stack, sem):
    pieces, half, _ = acts_ref.shape[1:]
    weight_copy = pltpu.make_async_copy(weight_hbm, weight, sem)
    weight_copy.start()

    def unpack(k, carry):
        upper = pl.ds(pl.multiple_of(k * 2 * half, 2 * half), half)
        lower = pl.ds(pl.multiple_of(k * 2 * half + half, half), half)
        for pair in range(2):
            lanes = pl.ds(pair * TILE, TILE)
            first, second = swap_halves(
                acts_ref[2 * pair, k].astype(jnp.float32), acts_ref[2 * pair + 1, k].astype(jnp.float32)
            )
            stack[upper, lanes] = first.astype(stack.dtype)
            stack[lower, lanes] = second.astype(stack.dtype)
        return carry

    lax.fori_loop(0, pieces, unpack, 0, unroll=True)

    bias_columns = bias_ref[...].T

    weight_copy.wait()
    for n in range(pieces * 2 * half // SPAN):
        base = n * SPAN
        for i in (1, 0):
            depth = (i + 1) * 512
            summed = jnp.dot(
                weight[i * 512 : (i + 1) * 512, :depth],
                stack[base : base + depth, :],
                preferred_element_type=jnp.float32,
            )
            for h in range(4):
                d = 4 * i + h
                mixed = summed[h * TILE : (h + 1) * TILE] + bias_columns[:, d : d + 1]
                stack[base + d * TILE : base + (d + 1) * TILE, :] = mixed.astype(stack.dtype)

    def repack(k, carry):
        upper = pl.ds(pl.multiple_of(k * 2 * half, 2 * half), half)
        lower = pl.ds(pl.multiple_of(k * 2 * half + half, half), half)
        for pair in range(2):
            lanes = pl.ds(pair * TILE, TILE)
            first, second = swap_halves(stack[upper, lanes].astype(jnp.float32), stack[lower, lanes].astype(jnp.float32))
            out_ref[2 * pair, k] = first.astype(out_ref.dtype)
            out_ref[2 * pair + 1, k] = second.astype(out_ref.dtype)
        return carry

    lax.fori_loop(0, pieces, repack, 0, unroll=True)


def gate_kernel(gate_ref, mixed_ref, out_hbm, out_ref, out_sems):
    rows, channels = gate_ref.shape
    half = rows // 2
    step = STEP

    def send(side, i):
        place = pl.ds(side * half + i * step, step)
        return pltpu.make_async_copy(out_ref.at[place], out_hbm.at[place], out_sems.at[side, i])

    def chunk(i, carry):
        top = pl.ds(pl.multiple_of(i * step, step), step)
        bottom = pl.ds(pl.multiple_of(half + i * step, step), step)
        for t in range(channels // TILE):
            lanes = pl.ds(t * TILE, TILE)
            upper, lower = swap_halves(
                mixed_ref[2 * t, top, :].astype(jnp.float32), mixed_ref[2 * t + 1, top, :].astype(jnp.float32)
            )
            for place, mixed in ((top, upper), (bottom, lower)):
                act = jax.nn.gelu(gate_ref[place, lanes].astype(jnp.float32))
                out_ref[place, lanes] = (act * mixed).astype(out_ref.dtype)
        for side in range(2):
            send(side, i).start()
        return carry

    lax.fori_loop(0, half // step, chunk, 0)
    for side, i in row_pieces(rows):
        send(side, i).wait()


def call(kernel, out_shape, specs, flops, moved, scratch=(), out_spec=VMEM, limit=16):
    if out_spec is VMEM:
        out = pltpu.VMEM(out_shape, jnp.bfloat16)
    else:
        out = jax.ShapeDtypeStruct(out_shape, jnp.bfloat16)
    return pl.pallas_call(
        kernel,
        out_shape=out,
        in_specs=specs,
        out_specs=out_spec,
        scratch_shapes=list(scratch),
        cost_estimate=pl.CostEstimate(flops=flops, bytes_accessed=moved, transcendentals=0),
        compiler_params=pltpu.CompilerParams(vmem_limit_bytes=limit << 20),
    )


def near(array):
    return pltpu.with_memory_space_constraint(array, pltpu.VMEM)


def copy_slots(rows):
    return pltpu.SemaphoreType.DMA((2, rows // 2 // STEP))


def local(gate_input, value_input, norm_gain, norm_bias, mix_weight, mix_bias):
    _, rows, channels = value_input.shape
    groups = channels // GROUP_DIM
    half = rows // 2
    x, core = lax.axis_index("x"), lax.axis_index("core")

    weight = mix_weight[0]
    excess = lax.ppermute(weight[:, 4 * TILE :], ("x", "core"), [(4, 3), (5, 2), (6, 1), (7, 0)])
    place = jnp.stack([2 * x + core]).astype(jnp.int32)
    folded = call(fold_kernel, (HALVES * HALF + 16, TILE), [SMEM, VMEM, VMEM, VMEM], 1000000, 600000)(
        place, weight, excess, mix_bias.reshape(SPAN // TILE, TILE)
    )
    quads = lax.all_gather(folded, "zq", axis=0)
    normed = call(
        norm_kernel,
        (groups, half, TILE),
        [VMEM, VMEM, VMEM],
        40000000,
        3200000,
        [pltpu.VMEM((64, channels), jnp.float32)],
        limit=60,
    )(value_input[0], norm_gain.reshape(1, channels), norm_bias.reshape(1, channels))
    normed, quads = lax.optimization_barrier((normed, quads))
    acts = lax.all_to_all(normed, QUAD, split_axis=0, concat_axis=0, tiled=True)

    received = []
    for s in range(4):
        piece = lax.dynamic_index_in_dim(quads, lax.rem(x + s, 4), 0, keepdims=False)
        received.append(lax.ppermute(piece, "x", [(i, (i + s) % 4) for i in range(4)]) if s else piece)
    own = jnp.stack(received)
    other = lax.ppermute(own, "core", [(0, 1), (1, 0)])

    full, bias_rows = pl.pallas_call(
        unfold_kernel,
        name="unfold",
        out_shape=(jax.ShapeDtypeStruct((SPAN, SPAN), jnp.bfloat16), pltpu.VMEM((8, TILE), jnp.float32)),
        in_specs=[SMEM, VMEM, VMEM],
        out_specs=(VMEM, VMEM),
        cost_estimate=pl.CostEstimate(flops=5000000, bytes_accessed=4000000, transcendentals=0),
        compiler_params=pltpu.CompilerParams(vmem_limit_bytes=16 << 20),
    )(jnp.stack([x, core]).astype(jnp.int32), near(own), near(other))
    mixed = call(
        mix_kernel,
        (4, groups // 4, half, TILE),
        [VMEM, HBM, VMEM],
        1000000000,
        6000000,
        [
            pltpu.VMEM((SPAN, SPAN), jnp.bfloat16),
            pltpu.VMEM((groups // 4 * rows, 2 * TILE), jnp.bfloat16),
            pltpu.SemaphoreType.DMA(()),
        ],
    )(near(acts.reshape(4, groups // 4, half, TILE)), pltpu.with_memory_space_constraint(full, pltpu.HBM), near(bias_rows))
    returned = lax.all_to_all(mixed.reshape(groups, half, TILE), QUAD, split_axis=0, concat_axis=0, tiled=True)

    gated = call(
        gate_kernel,
        (rows, channels),
        [VMEM, VMEM],
        40000000,
        4800000,
        [pltpu.VMEM((rows, channels), jnp.bfloat16), copy_slots(rows)],
        HBM,
    )(near(gate_input[0]), near(returned))
    return gated[None]


def solution(mesh):
    devices = mesh.devices.reshape(4, 4, 4, 4, 2)
    split = Mesh(devices, ("zq", "zr", "y", "x", "core"))
    sp, dp = ("zq", "zr", "y"), ("x", "core")
    in_specs = (P(dp, sp, None), P(dp, sp, None), P(), P(), P(sp, dp, None), P(sp, None))
    return jax.shard_map(local, mesh=split, in_specs=in_specs, out_specs=P(dp, sp, None), check_vma=False)
```
